32 devices in a mesh: ep: 8 (over z, x), tp: 4 (over y, core).
Axes of the slice: x: 2, y: 2, z: 4, core: 2. Of those that a mesh axis runs over, the one named last changes fastest.
Arguments:
- queries: bfloat16 [4096, 2048], P('ep', 'tp'), may hold values from -6 to 6
- keys_values: bfloat16 [4096, 4, 128], P('ep', 'tp'), may hold values from -12 to 12
- sinks: float32 [32], P('tp'), may hold values from 1 to 5
- tokens_b: bfloat16 [4096, 2048], P(('ep', 'tp')), may hold values from -6 to 6
- norm_gain: float32 [2048], replicated, may hold values from 0.1 to 1.9
- routes: int32 [4096, 2], P(('ep', 'tp')), may hold values from 0 to 7, all different within a row; in each aligned block of 128 rows (0 to 127, 128 to 255, ...) at most 40 rows name the same one
- route_weights: float32 [4096, 2], P(('ep', 'tp')), may hold values from 0.1 to 0.9
- gate_weight: bfloat16 [8, 2048, 3584], P('ep', None, 'tp'), may hold values from -0.125 to 0.125
- up_weight: bfloat16 [8, 2048, 3584], P('ep', None, 'tp'), may hold values from -0.125 to 0.125
- down_weight: bfloat16 [8, 3584, 2048], P('ep', 'tp'), may hold values from -0.09375 to 0.09375
Outputs:
- attended: bfloat16 [4096, 2048], P('ep', 'tp')
- moe_out: bfloat16 [4096, 2048], P(('ep', 'tp'))
The draws below stay inside these ranges and needn't reach their ends.
Inputs may be any that keep to these rules, and one draw needn't show every extreme that they name: `routes`: in each aligned block of 128 rows (the rows of one device) no expert is named by more than 40 rows; the 2 entries of a row differ.
All inputs are finite; a program needn't handle non-finite values.
Results may differ from the reference program's by a relative error of at most 0.012.
Values may be sent and summed in bfloat16 or wider, within the bound.
A program may use at most 128 MiB of HBM per device.

```python
import math
import jax
import jax.numpy as jnp
import numpy as np
from jax import lax

D = 2048
HEADS = 32
KV_HEADS = 4
HEAD = 64
WINDOW = 128
FFE = 3584
TOP = 2
TOKB_DEV = 128
EXPERTS = 8
CAP = 40
TOKENS_A = 4096
TOKENS_B = 4096
N_TP = 4


def draw_queries(key, part):
    shape = (TOKENS_A, HEADS * HEAD)
    base = jnp.clip(jax.random.normal(jax.random.fold_in(key, 11), shape, jnp.float32), -6.0, 6.0)
    return base.astype(jnp.bfloat16)


def draw_keys_values(key, part):
    shape = (TOKENS_A, KV_HEADS, HEAD)
    keys = jnp.clip(jax.random.normal(jax.random.fold_in(key, 13), shape, jnp.float32), -6.0, 6.0)
    values = jnp.clip(3.0 * jax.random.normal(jax.random.fold_in(key, 17), shape, jnp.float32), -12.0, 12.0)
    return jnp.concatenate([keys, values], axis=2).astype(jnp.bfloat16)


def level_of(rng, shape, pieces, smallest, high):
    factor_of, own = 1.0, jax.random.fold_in(rng, 6)
    for dim, blocks in pieces:
        steps = jnp.exp(jax.random.uniform(jax.random.fold_in(own, dim), (blocks,), jnp.float32, smallest / len(pieces), high / len(pieces)))
        factor_of = factor_of * jnp.repeat(steps, shape[dim] // blocks).reshape([-1 if axis == dim else 1 for axis in range(len(shape))])
    return factor_of


def routed_block(rng, own, number, rows, amount, top, limit, slope):
    sequence = jax.random.permutation(rng, amount)
    heavy_load, common = load_shares(amount, rows * top, limit, slope, True), load_shares(amount, rows * top, limit, slope, False)
    places = jnp.arange(amount)

    def named(lengths, offset_by):
        used = int((lengths > 0).sum())
        fixed = max(1, used // 4)
        passed = fixed + (places - fixed + offset_by * (used - fixed)) % max(1, amount - fixed)
        return jnp.zeros((amount,), jnp.int32).at[sequence[jnp.where(places < fixed, places, passed)]].set(jnp.asarray(lengths, jnp.int32))

    lengths = jnp.where(number % 4 == 0, named(heavy_load, number // 4), named(common, number - number // 4 - 1))
    mixed = jax.random.permutation(jax.random.fold_in(own, 3), amount)
    donor, sink = mixed[0:amount // 2 * 2:2], mixed[1:amount // 2 * 2:2]
    margin = jnp.minimum(lengths[donor] - 1, limit - lengths[sink]) // 2
    margin = jnp.where((donor == sequence[0]) | (sink == sequence[0]) | (lengths[sink] == 0), 0, jnp.maximum(margin, 0))
    passed = jax.random.randint(jax.random.fold_in(own, 4), (amount // 2,), 0, 1 << 20) % (margin + 1)
    lengths = lengths.at[donor].add(-passed).at[sink].add(passed)
    members = jnp.searchsorted(jnp.cumsum(lengths), jnp.arange(rows * top), side="right").astype(jnp.int32)
    table = members.reshape(top, rows).T
    table = table[jax.random.permutation(jax.random.fold_in(own, 1), rows)]
    offset_by = jax.random.randint(jax.random.fold_in(own, 2), (rows, 1), 0, top)
    return jnp.take_along_axis(table, (jnp.arange(top)[None, :] + offset_by) % top, axis=1)


def load_shares(count, total, bound, slope, full):
    portions = [(1 << 20) // math.isqrt(grade ** slope) + 1 for grade in range(1, count + 1)]
    largest = bound if full else min(bound, max(-(-total // count), total * portions[0] // sum(portions)))
    least = 1 if total - largest >= count - 1 else 0
    counts, surplus = [largest] + [least] * (count - 1), total - largest - least * (count - 1)
    while surplus > 0:
        free = [i for i in range(1, count) if counts[i] < largest] or [i for i in range(1, count) if counts[i] < bound]
        pool, budget = sum([portions[i] for i in free]), surplus
        for i in free:
            extra = min(bound - counts[i], max(1, budget * portions[i] // pool), surplus)
            counts[i] = counts[i] + extra
            surplus = surplus - extra
    return np.array(counts)


def centred(rng, shape, width, bound, split=(), kind=jnp.bfloat16):
    entries = jax.random.normal(rng, shape, jnp.float32) * width
    if len(split) > 0:
        entries = level_of(rng, shape, split, -0.22, 0.18) * entries
    return jnp.clip(entries, min=-bound, max=bound).astype(kind)


def setup_inputs(seed: int = 0) -> dict:
    splits = jax.random.split(jax.random.key(seed), 11)
    queries = draw_queries(jax.random.fold_in(splits[10], 71), 0)
    keys_values = draw_keys_values(jax.random.fold_in(splits[10], 71), 0)
    sinks = jnp.clip(1.0 + 4.0 * jax.random.uniform(splits[2], (HEADS,), jnp.float32) ** level_of(splits[2], (HEADS,), ((0, 4),), -0.2, 0.2), 1.0, 5.0)
    tokens_b = centred(splits[3], (TOKENS_B, D), 1.0, 6.0, ((0, 32),))
    norm_gain = jnp.clip(1.0 + 0.18 * jax.random.normal(splits[4], (D,), jnp.float32), 0.1, 1.9)
    routes_keys = jax.random.split(jax.random.fold_in(splits[5], 1), TOKENS_B // TOKB_DEV)
    routes_turns = jax.random.permutation(jax.random.fold_in(splits[5], 3), TOKENS_B // TOKB_DEV)
    routes = jax.vmap(lambda own, number: routed_block(jax.random.fold_in(splits[5], 2), own, number, TOKB_DEV, EXPERTS, TOP, CAP, 1))(routes_keys, routes_turns).reshape((TOKENS_B, TOP))
    route_weights = jnp.clip(0.1 + 0.79999997 * jax.random.uniform(splits[6], (TOKENS_B, TOP), jnp.float32) ** level_of(splits[6], (TOKENS_B, TOP), ((0, 32),), -0.2, 0.2), 0.1, 0.9)
    gate_weight = centred(splits[7], (EXPERTS, D, FFE), D ** -0.5, 0.125, ((0, 8), (2, 4)))
    up_weight = centred(splits[8], (EXPERTS, D, FFE), D ** -0.5, 0.125, ((0, 8), (2, 4)))
    down_weight = centred(splits[9], (EXPERTS, FFE, D), FFE ** -0.5, 0.09375, ((0, 8), (1, 4)))
    return dict(queries=queries, keys_values=keys_values, sinks=sinks, tokens_b=tokens_b, norm_gain=norm_gain, routes=routes, route_weights=route_weights, gate_weight=gate_weight, up_weight=up_weight, down_weight=down_weight)


NEG_SCORE = -1e+30
EPSILON = 1e-06

def attention_part(queries, keys_values, sinks):
    group_size = HEADS // KV_HEADS
    block_count = TOKENS_A // WINDOW
    padded_kv = jnp.concatenate([jnp.zeros((WINDOW, KV_HEADS, 2 * HEAD), jnp.bfloat16), keys_values], axis=0)
    head_ids = jnp.arange(HEADS, dtype=jnp.float32)
    slopes = (2.0 ** (-8.0 * (head_ids + 1.0) / HEADS)).reshape(KV_HEADS, group_size, 1, 1)
    sink_logit = sinks.reshape(KV_HEADS, group_size, 1, 1)
    query_pos = jnp.arange(WINDOW, dtype=jnp.int32)[:, None]
    key_pos = jnp.arange(2 * WINDOW, dtype=jnp.int32)[None, :]
    distance = WINDOW + query_pos - key_pos

    def one_block(block):
        query_rows = lax.dynamic_slice_in_dim(queries, block * WINDOW, WINDOW, 0)
        query_rows = query_rows.reshape(WINDOW, KV_HEADS, group_size, HEAD).astype(jnp.float32)
        near_kv = lax.dynamic_slice_in_dim(padded_kv, block * WINDOW, 2 * WINDOW, 0).astype(jnp.float32)
        keys = near_kv[:, :, :HEAD]
        values = near_kv[:, :, HEAD:]
        scores = jnp.einsum('qkgd,skd->kgqs', query_rows, keys) * HEAD ** (-0.5)
        key_global = (block - 1) * WINDOW + key_pos
        allowed = (distance >= 0) & (distance < WINDOW) & (key_global >= 0)
        scores = jnp.where(allowed, scores - slopes * distance.astype(jnp.float32), NEG_SCORE)
        peak_score = jnp.maximum(lax.optimization_barrier(jnp.max(scores, axis=-1, keepdims=True)), sink_logit)
        exponent = jnp.exp(scores - peak_score)
        denominator = lax.optimization_barrier(jnp.sum(exponent, axis=-1, keepdims=True)) + jnp.exp(sink_logit - peak_score)
        weights = (exponent / denominator).astype(jnp.bfloat16)
        mixed = jnp.einsum('kgqs,skd->qkgd', weights.astype(jnp.float32), values)
        return mixed.astype(jnp.bfloat16).reshape(WINDOW, HEADS * HEAD)
    blocks_out = lax.map(one_block, jnp.arange(block_count, dtype=jnp.int32))
    return blocks_out.reshape(TOKENS_A, HEADS * HEAD)

def expert_part(tokens_b, norm_gain, routes, route_weights, gate_weight, up_weight, down_weight):
    widened = tokens_b.astype(jnp.float32)
    scale = lax.rsqrt(lax.optimization_barrier(jnp.mean(widened * widened, axis=-1, keepdims=True)) + EPSILON)
    normed = (widened * scale * norm_gain).astype(jnp.bfloat16)
    source_count = TOKENS_B // TOKB_DEV
    pair_count = TOKB_DEV * TOP
    chosen = routes.reshape(source_count, pair_count)
    onehot = (chosen[:, :, None] == jnp.arange(EXPERTS, dtype=jnp.int32)).astype(jnp.int32)
    slots = lax.optimization_barrier(jnp.sum(jnp.cumsum(onehot, axis=1) * onehot, axis=2)) - 1
    row_width = source_count * CAP
    sources = jnp.arange(source_count, dtype=jnp.int32)[:, None]
    destination = chosen * row_width + sources * CAP + slots
    table = jnp.full((EXPERTS * row_width,), source_count * pair_count, jnp.int32)
    table = table.at[destination.reshape(-1)].set(jnp.arange(source_count * pair_count, dtype=jnp.int32))
    table = table.reshape(EXPERTS, row_width)
    flat_weights = jnp.concatenate([route_weights.reshape(-1), jnp.zeros((1,), jnp.float32)])
    padded = jnp.concatenate([normed, jnp.zeros((1, D), jnp.bfloat16)], axis=0)
    local_width = FFE // N_TP

    def expert_step(total, inputs):
        gate_w, up_w, down_w, picks = inputs
        token_ids = picks // TOP
        picked = padded[token_ids]
        gate_part = jnp.dot(picked, gate_w, preferred_element_type=jnp.float32)
        up_part = jnp.dot(picked, up_w, preferred_element_type=jnp.float32)
        hidden = (jax.nn.silu(gate_part) * up_part).astype(jnp.bfloat16)
        parts = jnp.einsum('rjf,jfd->jrd', hidden.reshape(row_width, N_TP, local_width).astype(jnp.float32), down_w.reshape(N_TP, local_width, D).astype(jnp.float32))
        parts = lax.optimization_barrier(parts.astype(jnp.bfloat16)).astype(jnp.float32)
        expert_out = lax.optimization_barrier(jnp.sum(parts, axis=0)).astype(jnp.bfloat16)
        scaled = flat_weights[picks][:, None] * expert_out.astype(jnp.float32)
        return (total.at[token_ids].add(scaled), None)
    start_total = jnp.zeros((TOKENS_B + 1, D), jnp.float32)
    total, _ = lax.scan(expert_step, start_total, (gate_weight, up_weight, down_weight, table))
    return total[:TOKENS_B].astype(jnp.bfloat16)

def reference(queries, keys_values, sinks, tokens_b, norm_gain, routes, route_weights, gate_weight, up_weight, down_weight):
    attended = attention_part(queries, keys_values, sinks)
    moe_out = expert_part(tokens_b, norm_gain, routes, route_weights, gate_weight, up_weight, down_weight)
    return (attended, moe_out)
```

```python
import functools

import jax
import jax.numpy as jnp
from jax import lax
from jax.experimental import pallas as pl
from jax.experimental.pallas import tpu as pltpu
from jax.sharding import PartitionSpec as P

WINDOW = 128
EPSILON = 1e-06
GROUPS = 8
SEND = (0, 1, 4, 5, 2, 6, 3, 7)
ORDER = (0, 1, 4, 2, 5, 3, 6, 7)
PLAN = (
    ("Y1", "F0"),
    ("Y4", "F1", "M0"),
    ("Y2", "F4"),
    ("Y5", "F2", "M4", "R0"),
    ("Y3", "F5"),
    ("Y6", "R4", "M5", "F3"),
    ("Y7", "F6"),
    ("R5", "M6", "M1", "F7"),
)
TAIL = ("R6", "M7", "M3", "M2", "R1", "R7", "K0", "K4", "R3", "K5", "R2", "K6", "K1", "K7", "K3", "K2")
MESH = pl.DeviceIdType.MESH
F32 = jnp.float32
BF16 = jnp.bfloat16


def remote(src, dst, send_sem, recv_sem, device):
    return pltpu.make_async_remote_copy(
        src_ref=src, dst_ref=dst, send_sem=send_sem, recv_sem=recv_sem,
        device_id=device, device_id_type=MESH,
    )


def kernel(
    n, m, cap, slot_rows,
    q_hbm, kv_hbm, sink_ref, tok_ref, gain_ref, routes_ref, rw_ref, wg_hbm, wu_hbm, wd_hbm,
    att_hbm, moe_hbm,
    att_ref, moe_ref, acc, q_ref, wg, wu, wd, kvx, out, piece, xb, hidden, parts, ra, qb, rb, fin, ret, comb,
    o_sem, w_sem, halo_sem, ep_send, ep_recv, y_send, y_recv, c_send, c_recv, d_send, d_recv,
    a_send, a_recv, b_send, b_recv, r_send, r_recv,
):
    p = lax.axis_index("ep")
    t = lax.axis_index("tp")
    t1 = t + 1 - 2 * (t % 2)
    t2 = (t + m // 2) % m
    t3 = (t1 + m // 2) % m
    per = n // GROUPS
    rows = m * per * slot_rows
    width = tok_ref.shape[1]
    hid = wg.shape[1]
    row_count = q_ref.shape[0]
    blocks = row_count // WINDOW

    def xor(a, b):
        total, bit = 0, 1
        while bit < n:
            total = total + ((a // bit + b // bit) % 2) * bit
            bit *= 2
        return total

    loads = [
        pltpu.make_async_copy(wg_hbm, wg, w_sem.at[0]),
        pltpu.make_async_copy(wu_hbm, wu, w_sem.at[1]),
        pltpu.make_async_copy(wd_hbm, wd, w_sem.at[2]),
    ]
    q_load = pltpu.make_async_copy(q_hbm, q_ref, w_sem.at[3])
    kv_load = pltpu.make_async_copy(kv_hbm, kvx.at[pl.ds(WINDOW, row_count)], w_sem.at[4])
    barrier = pltpu.get_barrier_semaphore()
    for s in range(1, n):
        pl.semaphore_signal(barrier, inc=1, device_id=(xor(p, s), t), device_id_type=MESH)
    pl.semaphore_signal(barrier, inc=1, device_id=(p, t1), device_id_type=MESH)
    pl.semaphore_signal(barrier, inc=1, device_id=(p, t2), device_id_type=MESH)

    kv_load.start()
    q_load.start()
    for load in loads:
        load.start()

    widened = tok_ref[...].astype(F32)
    scale = lax.rsqrt(jnp.mean(widened * widened, axis=-1, keepdims=True) + EPSILON)
    normed = (widened * scale * gain_ref[...]).astype(BF16)

    own = normed.shape[0]
    r0 = routes_ref[0:1, :]
    r1 = routes_ref[1:2, :]
    ids = lax.broadcasted_iota(jnp.int32, (max(n, 8), own), 0)
    is0 = ids == r0
    is1 = ids == r1
    member = jnp.where(is0 | is1, 1.0, 0.0).astype(BF16)
    rowi = lax.broadcasted_iota(jnp.int32, (own, own), 0)
    coli = lax.broadcasted_iota(jnp.int32, (own, own), 1)
    before = jnp.where(rowi < coli, 1.0, 0.0).astype(BF16)
    rank = jnp.dot(member, before, preferred_element_type=F32)
    k0 = jnp.sum(jnp.where(is0, rank, 0.0), axis=0, keepdims=True).astype(jnp.int32)
    k1 = jnp.sum(jnp.where(is1, rank, 0.0), axis=0, keepdims=True).astype(jnp.int32)
    e0 = jnp.bitwise_xor(r0, p) * slot_rows + k0
    e1 = jnp.bitwise_xor(r1, p) * slot_rows + k1
    slots = n * slot_rows
    slot_i = lax.broadcasted_iota(jnp.int32, (slots, own), 0)
    in0 = slot_i == e0
    in1 = slot_i == e1
    pick = jnp.where(in0 | in1, 1.0, 0.0).astype(BF16)
    weight = jnp.where(in0, rw_ref[0:1, :], 0.0) + jnp.where(in1, rw_ref[1:2, :], 0.0)
    for s in range(n):
        comb[s] = weight[s * slot_rows : (s + 1) * slot_rows].astype(BF16)
    def dispatch(s):
        return remote(out.at[s], piece.at[t, s], ep_send.at[s], ep_recv.at[s], (xor(p, s), t))

    def halo(to):
        return remote(kvx.at[pl.ds(row_count, WINDOW)], kvx.at[pl.ds(0, WINDOW)], halo_sem.at[0], halo_sem.at[1], (to, t))

    def part(g):
        return pl.ds(g * per, per)

    def y_copy(g):
        return remote(piece.at[t, part(g)], piece.at[t, part(g)], y_send.at[g], y_recv.at[g], (p, t2))

    def c_copy(g):
        return remote(piece.at[t, part(g)], piece.at[t, part(g)], c_send.at[g], c_recv.at[g], (p, t1))

    tile = min(512, width)
    for c in range(0, width, tile):
        block = jnp.dot(pick, normed[:, c : c + tile], preferred_element_type=F32)
        for s in range(n):
            out[s, :, c : c + tile] = block[s * slot_rows : (s + 1) * slot_rows].astype(BF16)
    piece[t, 0] = out[0]

    pl.semaphore_wait(barrier, n + 1)

    kv_load.wait()

    @pl.when(p < n - 1)
    def _():
        halo(p + 1).start()

    for g in SEND:
        for v in range(max(1, g * per), (g + 1) * per):
            dispatch(v).start()

    if per == 1:
        y_copy(0).start()
        c_copy(0).start()

    q_load.wait()

    @pl.when(p == 0)
    def _():
        kvx[0:WINDOW, :] = jnp.zeros((WINDOW, kvx.shape[1]), BF16)

    def d_copy(g):
        return remote(piece.at[t2, part(g)], piece.at[t2, part(g)], d_send.at[g], d_recv.at[g], (p, t1))

    def a_copy(i, g):
        return remote(parts.at[(t1, t3)[i], part(g)], ra.at[i, part(g)], a_send.at[i, g], a_recv.at[i, g], (p, t1))

    def b_copy(g):
        return remote(qb.at[part(g)], rb.at[part(g)], b_send.at[g], b_recv.at[g], (p, t2))

    def back(s):
        return remote(fin.at[s], ret.at[s], r_send.at[s], r_recv.at[s], (xor(p, s), t))

    def attention(b):
        head = kvx.shape[1] // 2
        local_heads = q_ref.shape[1] // head
        heads = local_heads * m
        near = kvx[pl.ds(pl.multiple_of(b * WINDOW, WINDOW), 2 * WINDOW), :]
        keys = (near[:, :head].astype(F32) * head ** (-0.5)).astype(BF16)
        ones = jnp.ones((2 * WINDOW, head), BF16)
        values = jnp.concatenate([near[:, head:], ones], axis=1)
        qi = lax.broadcasted_iota(jnp.int32, (WINDOW, 2 * WINDOW), 0)
        kj = lax.broadcasted_iota(jnp.int32, (WINDOW, 2 * WINDOW), 1)
        dist = WINDOW + qi - kj
        first = jnp.where(p + b == 0, WINDOW, 0)
        allowed = (dist >= 0) & (dist < WINDOW) & (kj >= first)
        dist_f = dist.astype(F32)
        at = pl.ds(pl.multiple_of(b * WINDOW, WINDOW), WINDOW)
        for pair in range(0, local_heads, 2):
            both = q_ref[at, pair * head : (pair + 2) * head]
            done = []
            for i in range(2):
                h = pair + i
                scores = lax.dot_general(
                    both[:, i * head : (i + 1) * head], keys, (((1,), (1,)), ((), ())),
                    preferred_element_type=F32,
                )
                ids = jnp.full((1, 2 * WINDOW), t * local_heads + h + 1, jnp.int32).astype(F32)
                slope = jnp.exp2(ids * (-8.0 / heads))
                scores = jnp.where(allowed, scores - slope * dist_f, -1e30)
                sink = sink_ref[h]
                peak = jnp.maximum(jnp.max(scores, axis=-1, keepdims=True), sink)
                weights = jnp.exp(scores - peak).astype(BF16)
                mixed = jnp.dot(weights, values, preferred_element_type=F32)
                total = mixed[:, head : head + 1] + jnp.exp(sink - peak)
                done.append(mixed[:, :head] / total)
            att_ref[at, pair * head : (pair + 2) * head] = jnp.concatenate(done, axis=1).astype(BF16)

    def experts(g):
        for o in range(m):
            for j in range(0, per):
                k = (o * per + j) * slot_rows
                xb[k : k + slot_rows, :] = piece[o, g * per + j]
        full = hid // 256 * 256
        x = xb[...]
        for c in range(0, full, 256):
            gate = jnp.dot(x, wg[:, c : c + 256], preferred_element_type=F32)
            up = jnp.dot(x, wu[:, c : c + 256], preferred_element_type=F32)
            hidden[:, c : c + 256] = (gate / (1.0 + jnp.exp(-gate)) * up).astype(BF16)
        if full < hid:
            tail = hid - full
            joint = jnp.concatenate([wg[:, full:], wu[:, full:]], axis=1)
            two = jnp.dot(x, joint, preferred_element_type=F32)
            gate, up = two[:, :tail], two[:, tail:]
            hidden[:, full:] = (gate / (1.0 + jnp.exp(-gate)) * up).astype(BF16)
        h = hidden[...]
        for c in range(0, width, 256):
            product = jnp.dot(h, wd[:, c : c + 256], preferred_element_type=F32)
            for o in range(m):
                for j in range(per):
                    k = (o * per + j) * slot_rows
                    parts[o, g * per + j, :, c : c + 256] = product[k : k + slot_rows].astype(BF16)

    across = (((0,), (0,)), ((), ()))
    att_out = pltpu.make_async_copy(att_ref, att_hbm, o_sem.at[0])

    def moe_out(i):
        cols = pl.ds(i * tile, tile)
        return pltpu.make_async_copy(moe_ref.at[:, cols], moe_hbm.at[:, cols], o_sem.at[1 + i])

    def spread(g):
        for v in range(max(1, g * per), (g + 1) * per):
            dispatch(v).wait_recv()
        y_copy(g).start()
        c_copy(g).start()

    def forward(g):
        y_copy(g).wait_recv()
        d_copy(g).start()

    def middle(g):
        a_copy(0, g).wait_recv()
        a_copy(1, g).wait_recv()
        for v in range(g * per, (g + 1) * per):
            qb[v] = (parts[t2, v].astype(F32) + ra[1, v].astype(F32)).astype(BF16)
        b_copy(g).start()

    def finish(g):
        b_copy(g).wait_recv()
        for v in range(g * per, (g + 1) * per):
            done = (parts[t, v].astype(F32) + ra[0, v].astype(F32) + rb[v].astype(F32)).astype(BF16)
            if v > 0:
                fin[v] = done
                back(v).start()
            else:
                ret[0] = done

    combined = [False]

    def combine(g, last):
        for v in range(g * per, (g + 1) * per):
            if v > 0:
                back(v).wait_recv()
            final = last and v == (g + 1) * per - 1
            for i in range(width // tile):
                c = i * tile
                term = lax.dot_general(comb[v], ret[v, :, c : c + tile], across, preferred_element_type=F32)
                if combined[0]:
                    term = acc[:, c : c + tile] + term
                if final:
                    moe_ref[:, c : c + tile] = term.astype(BF16)
                    moe_out(i).start()
                else:
                    acc[:, c : c + tile] = term
            combined[0] = True

    def run(ops, last):
        for op in ops:
            g = int(op[1:])
            if op[0] == "Y":
                spread(g)
            elif op[0] == "F":
                forward(g)
            elif op[0] == "M":
                middle(g)
            elif op[0] == "R":
                finish(g)
            else:
                combine(g, last and op == ops[-1])

    if per > 1:
        spread(0)

    @pl.loop(0, blocks)
    def _(b):
        @pl.when((b == blocks - 1) & (p > 0))
        def _():
            halo((p + 1) % n).wait_recv()

        attention(blocks - 1 - b)

    att_out.start()
    for load in loads:
        load.wait()

    def step(it, code):
        for k, ops in enumerate(PLAN):
            @pl.when(it == k)
            def _(ops=ops):
                run(ops, False)

        g = code % GROUPS
        c_copy(g).wait_recv()
        d_copy(g).wait_recv()
        experts(g)
        a_copy(0, g).start()
        a_copy(1, g).start()
        return code // GROUPS

    lax.fori_loop(0, GROUPS, step, jnp.int32(sum(g * GROUPS**k for k, g in enumerate(ORDER))))
    run(TAIL, True)
    att_out.wait()
    for i in range(width // tile):
        moe_out(i).wait()

    @pl.when(p < n - 1)
    def _():
        halo(p + 1).wait_send()

    @pl.loop(1, n)
    def _(s):
        dispatch(s).wait_send()
        back(s).wait_send()

    @pl.loop(0, GROUPS)
    def _(g):
        y_copy(g).wait_send()
        c_copy(g).wait_send()
        d_copy(g).wait_send()
        a_copy(0, g).wait_send()
        a_copy(1, g).wait_send()
        b_copy(g).wait_send()


def settle(attended_ref, moe_ref, attended_out, moe_out):
    attended_out[...] = attended_ref[...]
    moe_out[...] = moe_ref[...]


def local(n, m, queries, keys_values, sinks, tokens_b, norm_gain, routes, route_weights, gate_weight, up_weight, down_weight):
    own_rows, top_count = routes.shape
    width = tokens_b.shape[1]
    cap = max(2, 5 * own_rows * top_count // (4 * n))
    slot_rows = (cap + 7) // 8 * 8
    hid = gate_weight.shape[2]
    per = n // GROUPS
    rows = m * per * slot_rows
    vmem = pl.BlockSpec(memory_space=pltpu.VMEM)
    smem = pl.BlockSpec(memory_space=pltpu.SMEM)
    hbm = pl.BlockSpec(memory_space=pltpu.HBM)
    dma = pltpu.SemaphoreType.DMA
    attended, moe = pl.pallas_call(
        functools.partial(kernel, n, m, cap, slot_rows),
        out_shape=(
            jax.ShapeDtypeStruct(queries.shape, BF16),
            jax.ShapeDtypeStruct(tokens_b.shape, BF16),
        ),
        in_specs=[hbm, hbm, smem, vmem, vmem, vmem, vmem, hbm, hbm, hbm],
        out_specs=(hbm, hbm),
        scratch_shapes=[
            pltpu.VMEM(queries.shape, BF16),
            pltpu.VMEM(tokens_b.shape, BF16),
            pltpu.VMEM(tokens_b.shape, F32),
            pltpu.VMEM(queries.shape, BF16),
            pltpu.VMEM((width, hid), BF16),
            pltpu.VMEM((width, hid), BF16),
            pltpu.VMEM((hid, width), BF16),
            pltpu.VMEM((keys_values.shape[0] + WINDOW, keys_values.shape[2]), BF16),
            pltpu.VMEM((n, slot_rows, width), BF16),
            pltpu.VMEM((m, n, slot_rows, width), BF16),
            pltpu.VMEM((rows, width), BF16),
            pltpu.VMEM((rows, hid), BF16),
            pltpu.VMEM((m, n, slot_rows, width), BF16),
            pltpu.VMEM((2, n, slot_rows, width), BF16),
            pltpu.VMEM((n, slot_rows, width), BF16),
            pltpu.VMEM((n, slot_rows, width), BF16),
            pltpu.VMEM((n, slot_rows, width), BF16),
            pltpu.VMEM((n, slot_rows, width), BF16),
            pltpu.VMEM((n, slot_rows, own_rows), BF16),
            dma((1 + width // min(512, width),)), dma((5,)), dma((2,)), dma((n,)), dma((n,)),
            dma((GROUPS,)), dma((GROUPS,)), dma((GROUPS,)), dma((GROUPS,)), dma((GROUPS,)), dma((GROUPS,)),
            dma((2, GROUPS)), dma((2, GROUPS)), dma((GROUPS,)), dma((GROUPS,)), dma((n,)), dma((n,)),
        ],
        compiler_params=pltpu.CompilerParams(
            collective_id=0, has_side_effects=True, vmem_limit_bytes=62 * 1024 * 1024
        ),
    )(
        queries,
        keys_values.reshape(keys_values.shape[0], keys_values.shape[2]),
        sinks,
        tokens_b,
        norm_gain.reshape(1, width),
        routes.T,
        route_weights.T,
        gate_weight.reshape(width, hid),
        up_weight.reshape(width, hid),
        down_weight.reshape(hid, width),
    )
    return pl.pallas_call(
        settle,
        out_shape=(
            jax.ShapeDtypeStruct(queries.shape, BF16),
            jax.ShapeDtypeStruct(tokens_b.shape, BF16),
        ),
        in_specs=[vmem, vmem],
        out_specs=(vmem, vmem),
    )(attended, moe)


def solution(mesh):
    in_specs = (
        P("ep", "tp"),
        P("ep", "tp", None),
        P("tp"),
        P(("ep", "tp"), None),
        P(),
        P(("ep", "tp"), None),
        P(("ep", "tp"), None),
        P("ep", None, "tp"),
        P("ep", None, "tp"),
        P("ep", "tp", None),
    )
    out_specs = (P("ep", "tp"), P(("ep", "tp"), None))
    body = functools.partial(local, mesh.shape["ep"], mesh.shape["tp"])
    return jax.shard_map(body, mesh=mesh, in_specs=in_specs, out_specs=out_specs, check_vma=False)
```

```python
import functools

import jax
import jax.numpy as jnp
from jax import lax
from jax.experimental import pallas as pl
from jax.experimental.pallas import tpu as pltpu
from jax.sharding import PartitionSpec as P

WINDOW = 128
EPSILON = 1e-06
GROUPS = 8
NEAR = 4
FAR = (4, 6, 5, 7)
HELD = 0
INNER = 2
ORDER = (0, 4, 5, 1, 6, 2, 3, 7)
HEAD = ("P0", "P1", "Y4", "P2", "P3")
PLAN = (
    ("Y5",),
    ("F4", "Y6"),
    ("F5", "N1", "M4"),
    ("N2", "F6"),
    ("M5", "Y7", "R4"),
    ("N3",),
    ("M6", "R5"),
    ("M1", "F7"),
)
TAIL = ("R6", "M7", "M3", "M2", "M0", "R1", "R7", "R3", "K4", "R2", "R0")
TAIL += ("K0", "K1", "K5", "K6", "K7", "K3", "K2")
MESH = pl.DeviceIdType.MESH
F32 = jnp.float32
BF16 = jnp.bfloat16


def remote(src, dst, send_sem, recv_sem, device):
    return pltpu.make_async_remote_copy(
        src_ref=src, dst_ref=dst, send_sem=send_sem, recv_sem=recv_sem,
        device_id=device, device_id_type=MESH,
    )


def kernel(
    n, m, cap, slot_rows,
    q_hbm, kv_hbm, sink_ref, tok_ref, gain_ref, routes_ref, rw_ref, wg_hbm, wu_hbm, wd_hbm,
    att_hbm, moe_hbm,
    att_ref, moe_ref, acc, q_ref, wg, wu, wd, kvx, meta, nb, out, piece, xb, hidden, parts, ra, qb, rb, fin, ret,
    comb, pick2,
    o_sem, w_sem, halo_sem, ep_send, ep_recv, y_send, y_recv, c_send, c_recv, d_send, d_recv,
    a_send, a_recv, b_send, b_recv, r_send, r_recv, m_sem, n_send, n_recv,
):
    p = lax.axis_index("ep")
    t = lax.axis_index("tp")
    t1 = t + 1 - 2 * (t % 2)
    t2 = (t + m // 2) % m
    t3 = (t1 + m // 2) % m
    per = n // GROUPS
    near = NEAR * per
    tc = t % 2
    outer = 1 - (p // (n // 2) + p // (n // 4)) % 2
    width = tok_ref.shape[1]
    hid = wg.shape[1]
    row_count = q_ref.shape[0]
    blocks = row_count // WINDOW

    def xor(a, b):
        total, bit = 0, 1
        while bit < n:
            total = total + ((a // bit + b // bit) % 2) * bit
            bit *= 2
        return total

    loads = [
        pltpu.make_async_copy(wg_hbm, wg, w_sem.at[0]),
        pltpu.make_async_copy(wu_hbm, wu, w_sem.at[1]),
        pltpu.make_async_copy(wd_hbm, wd, w_sem.at[2]),
    ]
    q_load = pltpu.make_async_copy(q_hbm, q_ref, w_sem.at[3])
    kv_load = pltpu.make_async_copy(kv_hbm, kvx.at[pl.ds(WINDOW, row_count)], w_sem.at[4])
    barrier = pltpu.get_barrier_semaphore()
    for s in range(1, n):
        pl.semaphore_signal(barrier, inc=1, device_id=(xor(p, s), t), device_id_type=MESH)
    pl.semaphore_signal(barrier, inc=1, device_id=(p, t1), device_id_type=MESH)
    pl.semaphore_signal(barrier, inc=1, device_id=(p, t2), device_id_type=MESH)

    kv_load.start()
    q_load.start()
    for load in loads:
        load.start()

    widened = tok_ref[...].astype(F32)
    scale = lax.rsqrt(jnp.mean(widened * widened, axis=-1, keepdims=True) + EPSILON)
    normed = (widened * scale * gain_ref[...]).astype(BF16)

    own = normed.shape[0]
    nb[0] = normed
    r0 = routes_ref[0:1, :]
    r1 = routes_ref[1:2, :]
    ids = lax.broadcasted_iota(jnp.int32, (max(n, 8), own), 0)
    is0 = ids == r0
    is1 = ids == r1
    member = jnp.where(is0 | is1, 1.0, 0.0).astype(BF16)
    rowi = lax.broadcasted_iota(jnp.int32, (own, own), 0)
    coli = lax.broadcasted_iota(jnp.int32, (own, own), 1)
    before = jnp.where(rowi < coli, 1.0, 0.0).astype(BF16)
    rank = jnp.dot(member, before, preferred_element_type=F32)
    k0 = jnp.sum(jnp.where(is0, rank, 0.0), axis=0, keepdims=True).astype(jnp.int32)
    k1 = jnp.sum(jnp.where(is1, rank, 0.0), axis=0, keepdims=True).astype(jnp.int32)
    e0 = jnp.bitwise_xor(r0, p) * slot_rows + k0
    e1 = jnp.bitwise_xor(r1, p) * slot_rows + k1
    slots = n * slot_rows
    meta[0, 0:1] = e0.astype(F32)
    meta[0, 1:2] = e1.astype(F32)
    meta[0, 2:8] = jnp.zeros((6, own), F32)

    def place(which, count):
        info = meta[which]
        slot_i = lax.broadcasted_iota(jnp.int32, (count * slot_rows, own), 0).astype(F32)
        return slot_i == info[0:1], slot_i == info[1:2]

    in0, in1 = place(0, n)
    pick = jnp.where(in0 | in1, 1.0, 0.0).astype(BF16)
    weight = jnp.where(in0, rw_ref[0:1, :], 0.0) + jnp.where(in1, rw_ref[1:2, :], 0.0)
    for s in range(n):
        comb[s] = weight[s * slot_rows : (s + 1) * slot_rows].astype(BF16)

    def dispatch(s, half=0):
        sem = half * n + s
        return remote(
            out.at[s, half], piece.at[tc, s, half], ep_send.at[sem], ep_recv.at[sem], (xor(p, s), t)
        )

    def halo(to):
        return remote(kvx.at[pl.ds(row_count, WINDOW)], kvx.at[pl.ds(0, WINDOW)], halo_sem.at[0], halo_sem.at[1], (to, t))

    def part(g):
        return pl.ds(g * per, per)

    def y_copy(g):
        return remote(piece.at[tc, part(g), 0], piece.at[tc, part(g), 1], y_send.at[g], y_recv.at[g], (p, t2))

    def c_copy(g, whole):
        here = piece.at[tc, part(g)] if whole else piece.at[tc, part(g), 0]
        return remote(here, here, c_send.at[g], c_recv.at[g], (p, t1))

    tile = min(512, width)
    for c in range(0, width, tile):
        block = jnp.dot(pick, normed[:, c : c + tile], preferred_element_type=F32)
        for s in range(n):
            out[s, 0, :, c : c + tile] = block[s * slot_rows : (s + 1) * slot_rows].astype(BF16)
    piece[tc, 0, 0] = out[0, 0]

    def meta_copy():
        return remote(meta.at[0], meta.at[1], m_sem.at[0], m_sem.at[1], (p, t2))

    def token_copy(i):
        cols = pl.ds(i * tile, tile)
        return remote(nb.at[0, :, cols], nb.at[1, :, cols], n_send.at[i], n_recv.at[i], (p, t2))

    pl.semaphore_wait(barrier, n + 1)

    kv_load.wait()

    @pl.when(p < n - 1)
    def _():
        halo(p + 1).start()

    meta_copy().start()
    for i in range(width // tile - HELD):
        token_copy(i).start()

    def launch(groups, half):
        for g in groups:
            for v in range(max(1, g * per), (g + 1) * per):
                dispatch(v, half).start()

    launch((0, 1), 0)

    @pl.when(outer == 1)
    def _():
        launch(FAR, 0)

    launch((2, 3), 0)

    q_load.wait()

    @pl.when(p == 0)
    def _():
        kvx[0:WINDOW, :] = jnp.zeros((WINDOW, kvx.shape[1]), BF16)

    def d_copy(g):
        return remote(piece.at[tc, part(g), 1], piece.at[tc, part(g), 1], d_send.at[g], d_recv.at[g], (p, t1))

    def a_copy(g):
        return remote(parts.at[1 - tc, part(g)], ra.at[part(g)], a_send.at[g], a_recv.at[g], (p, t1))

    def b_copy(g):
        return remote(qb.at[part(g)], rb.at[part(g)], b_send.at[g], b_recv.at[g], (p, t2))

    def back(s):
        return remote(fin.at[s], ret.at[s], r_send.at[s], r_recv.at[s], (xor(p, s), t))

    def members(g):
        return [g * per + j for j in range(per) if not (isinstance(g, int) and g * per + j == 0)]

    def attention(b):
        head = kvx.shape[1] // 2
        local_heads = q_ref.shape[1] // head
        heads = local_heads * m
        near = kvx[pl.ds(pl.multiple_of(b * WINDOW, WINDOW), 2 * WINDOW), :]
        keys = (near[:, :head].astype(F32) * head ** (-0.5)).astype(BF16)
        ones = jnp.ones((2 * WINDOW, head), BF16)
        values = jnp.concatenate([near[:, head:], ones], axis=1)
        qi = lax.broadcasted_iota(jnp.int32, (WINDOW, 2 * WINDOW), 0)
        kj = lax.broadcasted_iota(jnp.int32, (WINDOW, 2 * WINDOW), 1)
        dist = WINDOW + qi - kj
        first = jnp.where(p + b == 0, WINDOW, 0)
        allowed = (dist >= 0) & (dist < WINDOW) & (kj >= first)
        dist_f = dist.astype(F32)
        at = pl.ds(pl.multiple_of(b * WINDOW, WINDOW), WINDOW)
        for pair in range(0, local_heads, 2):
            both = q_ref[at, pair * head : (pair + 2) * head]
            done = []
            for i in range(2):
                h = pair + i
                scores = lax.dot_general(
                    both[:, i * head : (i + 1) * head], keys, (((1,), (1,)), ((), ())),
                    preferred_element_type=F32,
                )
                ids = jnp.full((1, 2 * WINDOW), t * local_heads + h + 1, jnp.int32).astype(F32)
                slope = jnp.exp2(ids * (-8.0 / heads))
                scores = jnp.where(allowed, scores - slope * dist_f, -1e30)
                sink = sink_ref[h]
                peak = jnp.maximum(jnp.max(scores, axis=-1, keepdims=True), sink)
                weights = jnp.exp(scores - peak).astype(BF16)
                mixed = jnp.dot(weights, values, preferred_element_type=F32)
                total = mixed[:, head : head + 1] + jnp.exp(sink - peak)
                done.append(mixed[:, :head] / total)
            att_ref[at, pair * head : (pair + 2) * head] = jnp.concatenate(done, axis=1).astype(BF16)

    def experts(g):
        for o in range(m):
            for j in range(0, per):
                k = (o * per + j) * slot_rows
                xb[k : k + slot_rows, :] = piece[o // 2, g * per + j, o % 2]
        full = hid // 256 * 256
        x = xb[...]
        for c in range(0, full, 256):
            gate = jnp.dot(x, wg[:, c : c + 256], preferred_element_type=F32)
            up = jnp.dot(x, wu[:, c : c + 256], preferred_element_type=F32)
            hidden[:, c : c + 256] = (gate / (1.0 + jnp.exp(-gate)) * up).astype(BF16)
        if full < hid:
            tail = hid - full
            joint = jnp.concatenate([wg[:, full:], wu[:, full:]], axis=1)
            two = jnp.dot(x, joint, preferred_element_type=F32)
            gate, up = two[:, :tail], two[:, tail:]
            hidden[:, full:] = (gate / (1.0 + jnp.exp(-gate)) * up).astype(BF16)
        h = hidden[...]
        for c in range(0, width, 256):
            product = jnp.dot(h, wd[:, c : c + 256], preferred_element_type=F32)
            for o in range(m):
                for j in range(per):
                    k = (o * per + j) * slot_rows
                    parts[o // 2, g * per + j, o % 2, :, c : c + 256] = product[k : k + slot_rows].astype(BF16)

    across = (((0,), (0,)), ((), ()))
    att_out = pltpu.make_async_copy(att_ref, att_hbm, o_sem.at[0])

    def moe_out(i):
        cols = pl.ds(i * tile, tile)
        return pltpu.make_async_copy(moe_ref.at[:, cols], moe_hbm.at[:, cols], o_sem.at[1 + i])

    def peer(i):
        c = i * tile
        if i == 0:
            meta_copy().wait_recv()
            one0, one1 = place(1, near)
            pick2[0] = jnp.where(one0 | one1, 1.0, 0.0).astype(BF16)
        token_copy(i).wait_recv()
        block = jnp.dot(pick2[0], nb[1, :, c : c + tile], preferred_element_type=F32)
        for v in range(near):
            rows = block[v * slot_rows : (v + 1) * slot_rows].astype(BF16)
            if v > 0:
                out[v, 1, :, c : c + tile] = rows
            else:
                piece[tc, 0, 1, :, c : c + tile] = rows
        if i == INNER:
            @pl.when(outer == 0)
            def _():
                launch(FAR, 0)

        if i == width // tile - 1:
            launch((0, 1, 2, 3), 1)
            gather(0)

    def queue(i):
        token_copy(i).start()

    def gather(g):
        for v in members(g):
            dispatch(v).wait_recv()
            dispatch(v, 1).wait_recv()
        c_copy(g, True).start()

    def spread(g):
        for v in members(g):
            dispatch(v).wait_recv()
        y_copy(g).start()
        c_copy(g, False).start()

    def forward(g):
        y_copy(g).wait_recv()
        d_copy(g).start()

    def middle(g):
        a_copy(g).wait_recv()
        for j in range(per):
            v = g * per + j
            qb[v] = (parts[tc, v, 1].astype(F32) + ra[v, 1].astype(F32)).astype(BF16)
        b_copy(g).start()

    def finish(g):
        b_copy(g).wait_recv()
        for j in range(per):
            v = g * per + j
            done = (parts[tc, v, 0].astype(F32) + ra[v, 0].astype(F32) + rb[v].astype(F32)).astype(BF16)
            if isinstance(v, int) and v == 0:
                ret[0] = done
            else:
                fin[v] = done
                back(v).start()

    def actual(g):
        return g + (g // NEAR) * 2 * outer * (1 - 2 * ((g // 2) % 2))

    begun = [False]

    def combine(g, last):
        for j in range(per):
            v = g * per + j
            if not (isinstance(v, int) and v == 0):
                back(v).wait_recv()
            for i in range(width // tile):
                cols = slice(i * tile, (i + 1) * tile)
                term = lax.dot_general(comb[v], ret[v, :, cols], across, preferred_element_type=F32)
                if begun[0]:
                    term = acc[:, cols] + term
                if last and j == per - 1:
                    moe_ref[:, cols] = term.astype(BF16)
                    moe_out(i).start()
                else:
                    acc[:, cols] = term
            begun[0] = True

    def arrive(g, close):
        c_copy(g, close).wait_recv()
        if not close:
            d_copy(g).wait_recv()

    acts = dict(P=peer, Q=queue, N=gather, Y=spread, F=forward, M=middle, R=finish)

    def run(ops, last=False):
        for op in ops:
            g = int(op[1:])
            close = g < NEAR
            final = last and op == ops[-1]
            where = g if close else actual(g)
            if op[0] == "K":
                combine(where, final)
            elif op[0] == "E":
                arrive(where, close)
            else:
                acts[op[0]](where)

    @pl.loop(0, blocks)
    def _(b):
        @pl.when((b == blocks - 1) & (p > 0))
        def _():
            halo((p + 1) % n).wait_recv()

        attention(blocks - 1 - b)

    att_out.start()
    for load in loads:
        load.wait()

    run(HEAD)

    def step(it, code):
        for k, ops in enumerate(PLAN):
            @pl.when(it == k)
            def _(ops=ops + ("E%d" % ORDER[k],)):
                run(ops)

        g = actual(code % GROUPS)
        experts(g)
        a_copy(g).start()
        return code // GROUPS

    lax.fori_loop(0, GROUPS, step, jnp.int32(sum(g * GROUPS**k for k, g in enumerate(ORDER))))
    run(TAIL, True)
    att_out.wait()
    for i in range(width // tile):
        moe_out(i).wait()

    @pl.when(p < n - 1)
    def _():
        halo(p + 1).wait_send()

    meta_copy().wait_send()
    for i in range(width // tile):
        token_copy(i).wait_send()
    for s in range(1, n):
        dispatch(s).wait_send()
        back(s).wait_send()
        if s < near:
            dispatch(s, 1).wait_send()
    for g in range(GROUPS):
        c_copy(g, g < NEAR).wait_send()
        a_copy(g).wait_send()
        b_copy(g).wait_send()
        if g >= NEAR:
            y_copy(g).wait_send()
            d_copy(g).wait_send()


def settle(attended_ref, moe_ref, attended_out, moe_out):
    attended_out[...] = attended_ref[...]
    moe_out[...] = moe_ref[...]


def local(n, m, queries, keys_values, sinks, tokens_b, norm_gain, routes, route_weights, gate_weight, up_weight, down_weight):
    own_rows, top_count = routes.shape
    width = tokens_b.shape[1]
    cap = max(2, 5 * own_rows * top_count // (4 * n))
    slot_rows = (cap + 7) // 8 * 8
    hid = gate_weight.shape[2]
    per = n // GROUPS
    rows = m * per * slot_rows
    tiles = width // min(512, width)
    vmem = pl.BlockSpec(memory_space=pltpu.VMEM)
    smem = pl.BlockSpec(memory_space=pltpu.SMEM)
    hbm = pl.BlockSpec(memory_space=pltpu.HBM)
    dma = pltpu.SemaphoreType.DMA
    attended, moe = pl.pallas_call(
        functools.partial(kernel, n, m, cap, slot_rows),
        out_shape=(
            jax.ShapeDtypeStruct(queries.shape, BF16),
            jax.ShapeDtypeStruct(tokens_b.shape, BF16),
        ),
        in_specs=[hbm, hbm, smem, vmem, vmem, vmem, vmem, hbm, hbm, hbm],
        out_specs=(hbm, hbm),
        scratch_shapes=[
            pltpu.VMEM(queries.shape, BF16),
            pltpu.VMEM(tokens_b.shape, BF16),
            pltpu.VMEM(tokens_b.shape, F32),
            pltpu.VMEM(queries.shape, BF16),
            pltpu.VMEM((width, hid), BF16),
            pltpu.VMEM((width, hid), BF16),
            pltpu.VMEM((hid, width), BF16),
            pltpu.VMEM((keys_values.shape[0] + WINDOW, keys_values.shape[2]), BF16),
            pltpu.VMEM((2, 8, own_rows), F32),
            pltpu.VMEM((2, own_rows, width), BF16),
            pltpu.VMEM((n, 2, slot_rows, width), BF16),
            pltpu.VMEM((2, n, 2, slot_rows, width), BF16),
            pltpu.VMEM((rows, width), BF16),
            pltpu.VMEM((rows, hid), BF16),
            pltpu.VMEM((2, n, 2, slot_rows, width), BF16),
            pltpu.VMEM((n, 2, slot_rows, width), BF16),
            pltpu.VMEM((n, slot_rows, width), BF16),
            pltpu.VMEM((n, slot_rows, width), BF16),
            pltpu.VMEM((n, slot_rows, width), BF16),
            pltpu.VMEM((n, slot_rows, width), BF16),
            pltpu.VMEM((n, slot_rows, own_rows), BF16),
            pltpu.VMEM((1, NEAR * per * slot_rows, own_rows), BF16),
            dma((1 + tiles,)), dma((5,)), dma((2,)), dma((2 * n,)), dma((2 * n,)),
            dma((GROUPS,)), dma((GROUPS,)), dma((GROUPS,)), dma((GROUPS,)), dma((GROUPS,)), dma((GROUPS,)),
            dma((GROUPS,)), dma((GROUPS,)), dma((GROUPS,)), dma((GROUPS,)), dma((n,)), dma((n,)),
            dma((2,)), dma((tiles,)), dma((tiles,)),
        ],
        compiler_params=pltpu.CompilerParams(
            collective_id=0, has_side_effects=True, vmem_limit_bytes=62 * 1024 * 1024
        ),
    )(
        queries,
        keys_values.reshape(keys_values.shape[0], keys_values.shape[2]),
        sinks,
        tokens_b,
        norm_gain.reshape(1, width),
        routes.T,
        route_weights.T,
        gate_weight.reshape(width, hid),
        up_weight.reshape(width, hid),
        down_weight.reshape(hid, width),
    )
    return pl.pallas_call(
        settle,
        out_shape=(
            jax.ShapeDtypeStruct(queries.shape, BF16),
            jax.ShapeDtypeStruct(tokens_b.shape, BF16),
        ),
        in_specs=[vmem, vmem],
        out_specs=(vmem, vmem),
    )(attended, moe)


def solution(mesh):
    in_specs = (
        P("ep", "tp"),
        P("ep", "tp", None),
        P("tp"),
        P(("ep", "tp"), None),
        P(),
        P(("ep", "tp"), None),
        P(("ep", "tp"), None),
        P("ep", None, "tp"),
        P("ep", None, "tp"),
        P("ep", "tp", None),
    )
    out_specs = (P("ep", "tp"), P(("ep", "tp"), None))
    body = functools.partial(local, mesh.shape["ep"], mesh.shape["tp"])
    return jax.shard_map(body, mesh=mesh, in_specs=in_specs, out_specs=out_specs, check_vma=False)
```

```python
import functools

import jax
import jax.numpy as jnp
from jax import lax
from jax.experimental import pallas as pl
from jax.experimental.pallas import tpu as pltpu
from jax.sharding import PartitionSpec as P

WINDOW = 128
EPSILON = 1e-06
GROUPS = 8
NEAR = 4
OUTER_FAR = (6, 4, 5, 7)
INNER_FAR = (4, 6, 7, 5)
PARTS = 2
HELD = 0
INNER = 2
ORDER = (0, 4, 5, 1, 6, 2, 3, 7)
HEAD = ("P0", "P1", "Y4", "P2", "P3")
PLAN = (
    ("Y5",),
    ("F4", "Y6"),
    ("F5", "N1", "M4"),
    ("N2", "F6"),
    ("M5", "Y7", "R4"),
    ("N3",),
    ("R5", "M6"),
    ("M1", "F7"),
)
TAIL = ("R6", "M7", "M3", "M2", "M0", "R1", "R7", "R3", "K4")
TAIL += ("R2", "R0", "S0", "K0", "K1", "K5", "K6", "K7", "K3", "K2")
MESH = pl.DeviceIdType.MESH
F32 = jnp.float32
BF16 = jnp.bfloat16


def remote(src, dst, send_sem, recv_sem, device):
    return pltpu.make_async_remote_copy(
        src_ref=src, dst_ref=dst, send_sem=send_sem, recv_sem=recv_sem,
        device_id=device, device_id_type=MESH,
    )


def kernel(
    n, m, cap, slot_rows,
    q_hbm, kv_hbm, sink_hbm, tok_hbm, gain_hbm, routes_hbm, rw_hbm, wg_hbm, wu_hbm, wd_hbm,
    att_hbm, moe_hbm,
    sink_ref, tok_ref, gain_ref, routes_ref, rw_ref, i_sem,
    att_ref, moe_ref, acc, q_ref, wg, wu, wd, kvx, meta, nb, out, piece, xb, hidden, parts, ra, qb, rb, fin, ret,
    comb, pick2,
    o_sem, w_sem, halo_sem, ep_send, ep_recv, y_send, y_recv, c_send, c_recv, d_send, d_recv,
    a_send, a_recv, b_send, b_recv, r_send, r_recv, m_sem, n_send, n_recv,
):
    p = lax.axis_index("ep")
    t = lax.axis_index("tp")
    t1 = t + 1 - 2 * (t % 2)
    t2 = (t + m // 2) % m
    t3 = (t1 + m // 2) % m
    per = n // GROUPS
    near = NEAR * per
    tc = t % 2
    part_width = tok_ref.shape[1] // PARTS
    outer = 1 - (p // (n // 2) + p // (n // 4)) % 2
    width = tok_ref.shape[1]
    hid = wg.shape[1]
    row_count = q_ref.shape[0]
    blocks = row_count // WINDOW

    def xor(a, b):
        total, bit = 0, 1
        while bit < n:
            total = total + ((a // bit + b // bit) % 2) * bit
            bit *= 2
        return total

    loads = [
        pltpu.make_async_copy(wg_hbm, wg, w_sem.at[0]),
        pltpu.make_async_copy(wu_hbm, wu, w_sem.at[1]),
        pltpu.make_async_copy(wd_hbm, wd, w_sem.at[2]),
    ]
    q_load = pltpu.make_async_copy(q_hbm, q_ref, w_sem.at[3])
    kv_load = pltpu.make_async_copy(kv_hbm, kvx.at[pl.ds(WINDOW, row_count)], w_sem.at[4])
    early = [
        pltpu.make_async_copy(source, target, i_sem.at[i])
        for i, (source, target) in enumerate((
            (tok_hbm, tok_ref), (gain_hbm, gain_ref), (routes_hbm, routes_ref), (rw_hbm, rw_ref), (sink_hbm, sink_ref),
        ))
    ]
    for load in early:
        load.start()
    barrier = pltpu.get_barrier_semaphore()
    for s in range(1, n):
        pl.semaphore_signal(barrier, inc=1, device_id=(xor(p, s), t), device_id_type=MESH)
    pl.semaphore_signal(barrier, inc=1, device_id=(p, t1), device_id_type=MESH)
    pl.semaphore_signal(barrier, inc=1, device_id=(p, t2), device_id_type=MESH)

    kv_load.start()
    q_load.start()
    for load in loads:
        load.start()

    for load in early:
        load.wait()
    widened = tok_ref[...].astype(F32)
    scale = lax.rsqrt(jnp.mean(widened * widened, axis=-1, keepdims=True) + EPSILON)
    normed = (widened * scale * gain_ref[...]).astype(BF16)

    own = normed.shape[0]
    nb[0] = normed
    r0 = routes_ref[0:1, :]
    r1 = routes_ref[1:2, :]
    ids = lax.broadcasted_iota(jnp.int32, (max(n, 8), own), 0)
    is0 = ids == r0
    is1 = ids == r1
    member = jnp.where(is0 | is1, 1.0, 0.0).astype(BF16)
    rowi = lax.broadcasted_iota(jnp.int32, (own, own), 0)
    coli = lax.broadcasted_iota(jnp.int32, (own, own), 1)
    before = jnp.where(rowi < coli, 1.0, 0.0).astype(BF16)
    rank = jnp.dot(member, before, preferred_element_type=F32)
    k0 = jnp.sum(jnp.where(is0, rank, 0.0), axis=0, keepdims=True).astype(jnp.int32)
    k1 = jnp.sum(jnp.where(is1, rank, 0.0), axis=0, keepdims=True).astype(jnp.int32)
    e0 = jnp.bitwise_xor(r0, p) * slot_rows + k0
    e1 = jnp.bitwise_xor(r1, p) * slot_rows + k1
    slots = n * slot_rows
    meta[0, 0:1] = e0.astype(F32)
    meta[0, 1:2] = e1.astype(F32)
    meta[0, 2:8] = jnp.zeros((6, own), F32)

    def place(which, count):
        info = meta[which]
        slot_i = lax.broadcasted_iota(jnp.int32, (count * slot_rows, own), 0).astype(F32)
        return slot_i == info[0:1], slot_i == info[1:2]

    in0, in1 = place(0, n)
    pick = jnp.where(in0 | in1, 1.0, 0.0).astype(BF16)
    weight = jnp.where(in0, rw_ref[0:1, :], 0.0) + jnp.where(in1, rw_ref[1:2, :], 0.0)
    for s in range(n):
        comb[s] = weight[s * slot_rows : (s + 1) * slot_rows].astype(BF16)

    def dispatch(s, half=0):
        sem = half * n + s
        return remote(
            out.at[s, half], piece.at[tc, s, half], ep_send.at[sem], ep_recv.at[sem], (xor(p, s), t)
        )

    def halo(to):
        return remote(kvx.at[pl.ds(row_count, WINDOW)], kvx.at[pl.ds(0, WINDOW)], halo_sem.at[0], halo_sem.at[1], (to, t))

    def part(g):
        return pl.ds(g * per, per)

    def y_copy(g):
        return remote(piece.at[tc, part(g), 0], piece.at[tc, part(g), 1], y_send.at[g], y_recv.at[g], (p, t2))

    def c_copy(g, whole):
        here = piece.at[tc, part(g)] if whole else piece.at[tc, part(g), 0]
        return remote(here, here, c_send.at[g], c_recv.at[g], (p, t1))

    tile = min(512, width)
    for c in range(0, width, tile):
        block = jnp.dot(pick, normed[:, c : c + tile], preferred_element_type=F32)
        for s in range(n):
            out[s, 0, :, c : c + tile] = block[s * slot_rows : (s + 1) * slot_rows].astype(BF16)
    piece[tc, 0, 0] = out[0, 0]

    def meta_copy():
        return remote(meta.at[0], meta.at[1], m_sem.at[0], m_sem.at[1], (p, t2))

    def token_copy(i):
        cols = pl.ds(i * tile, tile)
        return remote(nb.at[0, :, cols], nb.at[1, :, cols], n_send.at[i], n_recv.at[i], (p, t2))

    pl.semaphore_wait(barrier, n + 1)

    kv_load.wait()

    @pl.when(p < n - 1)
    def _():
        halo(p + 1).start()

    meta_copy().start()
    for i in range(width // tile - HELD):
        token_copy(i).start()

    def launch(groups, half):
        for g in groups:
            for v in range(max(1, g * per), (g + 1) * per):
                dispatch(v, half).start()

    launch((0, 1), 0)

    @pl.when(outer == 1)
    def _():
        launch(OUTER_FAR, 0)

    launch((2, 3), 0)

    q_load.wait()

    @pl.when(p == 0)
    def _():
        kvx[0:WINDOW, :] = jnp.zeros((WINDOW, kvx.shape[1]), BF16)

    def d_copy(g):
        return remote(piece.at[tc, part(g), 1], piece.at[tc, part(g), 1], d_send.at[g], d_recv.at[g], (p, t1))

    def a_copy(g):
        return remote(parts.at[1 - tc, part(g)], ra.at[part(g)], a_send.at[g], a_recv.at[g], (p, t1))

    def b_copy(g, h):
        cols = pl.ds(h * part_width, part_width)
        return remote(
            qb.at[part(g), :, cols], rb.at[part(g), :, cols], b_send.at[h, g], b_recv.at[h, g], (p, t2)
        )

    def back(s, h):
        cols = pl.ds(h * part_width, part_width)
        return remote(
            fin.at[s, :, cols], ret.at[s, :, cols], r_send.at[h, s], r_recv.at[h, s], (xor(p, s), t)
        )

    def members(g):
        return [g * per + j for j in range(per) if not (isinstance(g, int) and g * per + j == 0)]

    def attention(b):
        head = kvx.shape[1] // 2
        local_heads = q_ref.shape[1] // head
        heads = local_heads * m
        near = kvx[pl.ds(pl.multiple_of(b * WINDOW, WINDOW), 2 * WINDOW), :]
        keys = (near[:, :head].astype(F32) * head ** (-0.5)).astype(BF16)
        ones = jnp.ones((2 * WINDOW, head), BF16)
        values = jnp.concatenate([near[:, head:], ones], axis=1)
        qi = lax.broadcasted_iota(jnp.int32, (WINDOW, 2 * WINDOW), 0)
        kj = lax.broadcasted_iota(jnp.int32, (WINDOW, 2 * WINDOW), 1)
        dist = WINDOW + qi - kj
        first = jnp.where(p + b == 0, WINDOW, 0)
        allowed = (dist >= 0) & (dist < WINDOW) & (kj >= first)
        dist_f = dist.astype(F32)
        at = pl.ds(pl.multiple_of(b * WINDOW, WINDOW), WINDOW)
        for pair in range(0, local_heads, 2):
            both = q_ref[at, pair * head : (pair + 2) * head]
            done = []
            for i in range(2):
                h = pair + i
                scores = lax.dot_general(
                    both[:, i * head : (i + 1) * head], keys, (((1,), (1,)), ((), ())),
                    preferred_element_type=F32,
                )
                ids = jnp.full((1, 2 * WINDOW), t * local_heads + h + 1, jnp.int32).astype(F32)
                slope = jnp.exp2(ids * (-8.0 / heads))
                scores = jnp.where(allowed, scores - slope * dist_f, -1e30)
                sink = sink_ref[h]
                peak = jnp.maximum(jnp.max(scores, axis=-1, keepdims=True), sink)
                weights = jnp.exp(scores - peak).astype(BF16)
                mixed = jnp.dot(weights, values, preferred_element_type=F32)
                total = mixed[:, head : head + 1] + jnp.exp(sink - peak)
                done.append(mixed[:, :head] / total)
            att_ref[at, pair * head : (pair + 2) * head] = jnp.concatenate(done, axis=1).astype(BF16)

    def experts(g):
        for o in range(m):
            for j in range(0, per):
                k = (o * per + j) * slot_rows
                xb[k : k + slot_rows, :] = piece[o // 2, g * per + j, o % 2]
        full = hid // 256 * 256
        x = xb[...]
        for c in range(0, full, 256):
            gate = jnp.dot(x, wg[:, c : c + 256], preferred_element_type=F32)
            up = jnp.dot(x, wu[:, c : c + 256], preferred_element_type=F32)
            hidden[:, c : c + 256] = (gate / (1.0 + jnp.exp(-gate)) * up).astype(BF16)
        if full < hid:
            tail = hid - full
            joint = jnp.concatenate([wg[:, full:], wu[:, full:]], axis=1)
            two = jnp.dot(x, joint, preferred_element_type=F32)
            gate, up = two[:, :tail], two[:, tail:]
            hidden[:, full:] = (gate / (1.0 + jnp.exp(-gate)) * up).astype(BF16)
        h = hidden[...]
        for c in range(0, width, 256):
            product = jnp.dot(h, wd[:, c : c + 256], preferred_element_type=F32)
            for o in range(m):
                for j in range(per):
                    k = (o * per + j) * slot_rows
                    parts[o // 2, g * per + j, o % 2, :, c : c + 256] = product[k : k + slot_rows].astype(BF16)

    across = (((0,), (0,)), ((), ()))
    att_out = pltpu.make_async_copy(att_ref, att_hbm, o_sem.at[0])

    def moe_out(i):
        cols = pl.ds(i * tile, tile)
        return pltpu.make_async_copy(moe_ref.at[:, cols], moe_hbm.at[:, cols], o_sem.at[1 + i])

    def peer(i):
        c = i * tile
        if i == 0:
            meta_copy().wait_recv()
            one0, one1 = place(1, near)
            pick2[0] = jnp.where(one0 | one1, 1.0, 0.0).astype(BF16)
        token_copy(i).wait_recv()
        block = jnp.dot(pick2[0], nb[1, :, c : c + tile], preferred_element_type=F32)
        for v in range(near):
            rows = block[v * slot_rows : (v + 1) * slot_rows].astype(BF16)
            if v > 0:
                out[v, 1, :, c : c + tile] = rows
            else:
                piece[tc, 0, 1, :, c : c + tile] = rows
        if i == INNER:
            @pl.when(outer == 0)
            def _():
                launch(INNER_FAR, 0)

        if i == width // tile - 1:
            launch((0, 1, 2, 3), 1)
            gather(0)

    def queue(i):
        token_copy(i).start()

    def gather(g):
        for v in members(g):
            dispatch(v).wait_recv()
            dispatch(v, 1).wait_recv()
        c_copy(g, True).start()

    def spread(g):
        for v in members(g):
            dispatch(v).wait_recv()
        y_copy(g).start()
        c_copy(g, False).start()

    def forward(g):
        y_copy(g).wait_recv()
        d_copy(g).start()

    def middle(g):
        a_copy(g).wait_recv()
        for h in range(PARTS):
            cols = slice(h * part_width, (h + 1) * part_width)
            for j in range(per):
                v = g * per + j
                mine = parts[tc, v, 1, :, cols].astype(F32)
                qb[v, :, cols] = (mine + ra[v, 1, :, cols].astype(F32)).astype(BF16)
            b_copy(g, h).start()

    def finish(g):
        for h in range(PARTS):
            cols = slice(h * part_width, (h + 1) * part_width)
            b_copy(g, h).wait_recv()
            for j in range(per):
                v = g * per + j
                mine = parts[tc, v, 0, :, cols].astype(F32) + ra[v, 0, :, cols].astype(F32)
                done = (mine + rb[v, :, cols].astype(F32)).astype(BF16)
                if isinstance(v, int) and v == 0:
                    ret[0, :, cols] = done
                else:
                    fin[v, :, cols] = done
                    back(v, h).start()

    def actual(g):
        return g + (g // NEAR) * 2 * outer * (1 - 2 * ((g // 2) % 2))

    begun = [False]

    def combine(g, last):
        for j in range(per):
            v = g * per + j
            for i in range(width // tile):
                if not (isinstance(v, int) and v == 0) and i * tile % part_width == 0:
                    back(v, i * tile // part_width).wait_recv()
                cols = slice(i * tile, (i + 1) * tile)
                term = lax.dot_general(comb[v], ret[v, :, cols], across, preferred_element_type=F32)
                if begun[0]:
                    term = acc[:, cols] + term
                if last and j == per - 1:
                    moe_ref[:, cols] = term.astype(BF16)
                    moe_out(i).start()
                else:
                    acc[:, cols] = term
            begun[0] = True

    def arrive(g, close):
        c_copy(g, close).wait_recv()
        if not close:
            d_copy(g).wait_recv()

    def drain(_):
        @pl.when(p < n - 1)
        def _():
            halo(p + 1).wait_send()

        meta_copy().wait_send()
        for i in range(width // tile):
            token_copy(i).wait_send()
        for s in range(1, n):
            dispatch(s).wait_send()
            if s < near:
                dispatch(s, 1).wait_send()
        for g in range(GROUPS):
            c_copy(g, g < NEAR).wait_send()
            a_copy(g).wait_send()
            for h in range(PARTS):
                b_copy(g, h).wait_send()
            if g >= NEAR:
                y_copy(g).wait_send()
                d_copy(g).wait_send()

    acts = dict(S=drain, P=peer, Q=queue, N=gather, Y=spread, F=forward, M=middle, R=finish)

    def run(ops, last=False):
        for op in ops:
            g = int(op[1:])
            close = g < NEAR
            final = last and op == ops[-1]
            where = g if close else actual(g)
            if op[0] == "K":
                combine(where, final)
            elif op[0] == "E":
                arrive(where, close)
            else:
                acts[op[0]](where)

    @pl.loop(0, blocks)
    def _(b):
        @pl.when((b == blocks - 1) & (p > 0))
        def _():
            halo((p + 1) % n).wait_recv()

        attention(blocks - 1 - b)

    att_out.start()
    for load in loads:
        load.wait()

    run(HEAD)

    def step(it, code):
        for k, ops in enumerate(PLAN):
            @pl.when(it == k)
            def _(ops=ops + ("E%d" % ORDER[k],)):
                run(ops)

        g = actual(code % GROUPS)
        experts(g)
        a_copy(g).start()
        return code // GROUPS

    lax.fori_loop(0, GROUPS, step, jnp.int32(sum(g * GROUPS**k for k, g in enumerate(ORDER))))
    run(TAIL, True)
    att_out.wait()
    for i in range(width // tile):
        moe_out(i).wait()

    for s in range(1, n):
        for h in range(PARTS):
            back(s, h).wait_send()


def settle(attended_hbm, moe_hbm, attended_out, moe_out, attended_ref, moe_ref, sem):
    loads, stores = [], []
    for source, held, target in ((attended_hbm, attended_ref, attended_out), (moe_hbm, moe_ref, moe_out)):
        step = source.shape[0] // 2
        for i in range(2):
            at = pl.ds(i * step, step)
            loads.append(pltpu.make_async_copy(source.at[at], held.at[at], sem.at[0, len(loads)]))
            stores.append(pltpu.make_async_copy(held.at[at], target.at[at], sem.at[1, len(stores)]))
    for load in loads:
        load.start()
    for load, store in zip(loads, stores):
        load.wait()
        store.start()
    for store in stores:
        store.wait()


def local(n, m, queries, keys_values, sinks, tokens_b, norm_gain, routes, route_weights, gate_weight, up_weight, down_weight):
    own_rows, top_count = routes.shape
    width = tokens_b.shape[1]
    cap = max(2, 5 * own_rows * top_count // (4 * n))
    slot_rows = (cap + 7) // 8 * 8
    hid = gate_weight.shape[2]
    per = n // GROUPS
    rows = m * per * slot_rows
    tiles = width // min(512, width)
    hbm = pl.BlockSpec(memory_space=pltpu.HBM)
    dma = pltpu.SemaphoreType.DMA
    attended, moe = pl.pallas_call(
        functools.partial(kernel, n, m, cap, slot_rows),
        out_shape=(
            jax.ShapeDtypeStruct(queries.shape, BF16),
            jax.ShapeDtypeStruct(tokens_b.shape, BF16),
        ),
        in_specs=[hbm] * 10,
        out_specs=(hbm, hbm),
        scratch_shapes=[
            pltpu.SMEM(sinks.shape, F32),
            pltpu.VMEM(tokens_b.shape, BF16),
            pltpu.VMEM((1, width), F32),
            pltpu.VMEM((top_count, own_rows), jnp.int32),
            pltpu.VMEM((top_count, own_rows), F32),
            dma((5,)),
            pltpu.VMEM(queries.shape, BF16),
            pltpu.VMEM(tokens_b.shape, BF16),
            pltpu.VMEM(tokens_b.shape, F32),
            pltpu.VMEM(queries.shape, BF16),
            pltpu.VMEM((width, hid), BF16),
            pltpu.VMEM((width, hid), BF16),
            pltpu.VMEM((hid, width), BF16),
            pltpu.VMEM((keys_values.shape[0] + WINDOW, keys_values.shape[2]), BF16),
            pltpu.VMEM((2, 8, own_rows), F32),
            pltpu.VMEM((2, own_rows, width), BF16),
            pltpu.VMEM((n, 2, slot_rows, width), BF16),
            pltpu.VMEM((2, n, 2, slot_rows, width), BF16),
            pltpu.VMEM((rows, width), BF16),
            pltpu.VMEM((rows, hid), BF16),
            pltpu.VMEM((2, n, 2, slot_rows, width), BF16),
            pltpu.VMEM((n, 2, slot_rows, width), BF16),
            pltpu.VMEM((n, slot_rows, width), BF16),
            pltpu.VMEM((n, slot_rows, width), BF16),
            pltpu.VMEM((n, slot_rows, width), BF16),
            pltpu.VMEM((n, slot_rows, width), BF16),
            pltpu.VMEM((n, slot_rows, own_rows), BF16),
            pltpu.VMEM((1, NEAR * per * slot_rows, own_rows), BF16),
            dma((1 + tiles,)), dma((5,)), dma((2,)), dma((2 * n,)), dma((2 * n,)),
            dma((GROUPS,)), dma((GROUPS,)), dma((GROUPS,)), dma((GROUPS,)), dma((GROUPS,)), dma((GROUPS,)),
            dma((GROUPS,)), dma((GROUPS,)), dma((PARTS, GROUPS)), dma((PARTS, GROUPS)),
            dma((PARTS, n)), dma((PARTS, n)),
            dma((2,)), dma((tiles,)), dma((tiles,)),
        ],
        compiler_params=pltpu.CompilerParams(
            collective_id=0, has_side_effects=True, vmem_limit_bytes=62 * 1024 * 1024
        ),
    )(
        queries,
        keys_values.reshape(keys_values.shape[0], keys_values.shape[2]),
        sinks,
        tokens_b,
        norm_gain.reshape(1, width),
        routes.T,
        route_weights.T,
        gate_weight.reshape(width, hid),
        up_weight.reshape(width, hid),
        down_weight.reshape(hid, width),
    )
    return pl.pallas_call(
        settle,
        out_shape=(
            jax.ShapeDtypeStruct(queries.shape, BF16),
            jax.ShapeDtypeStruct(tokens_b.shape, BF16),
        ),
        in_specs=[hbm, hbm],
        out_specs=(hbm, hbm),
        scratch_shapes=[
            pltpu.VMEM(queries.shape, BF16),
            pltpu.VMEM(tokens_b.shape, BF16),
            dma((2, 4)),
        ],
    )(attended, moe)


def solution(mesh):
    in_specs = (
        P("ep", "tp"),
        P("ep", "tp", None),
        P("tp"),
        P(("ep", "tp"), None),
        P(),
        P(("ep", "tp"), None),
        P(("ep", "tp"), None),
        P("ep", None, "tp"),
        P("ep", None, "tp"),
        P("ep", "tp", None),
    )
    out_specs = (P("ep", "tp"), P(("ep", "tp"), None))
    body = functools.partial(local, mesh.shape["ep"], mesh.shape["tp"])
    return jax.shard_map(body, mesh=mesh, in_specs=in_specs, out_specs=out_specs, check_vma=False)
```

```python
import functools

import jax
import jax.numpy as jnp
from jax import lax
from jax.experimental import pallas as pl
from jax.experimental.pallas import tpu as pltpu
from jax.sharding import PartitionSpec as P

WINDOW = 128
EPSILON = 1e-06
GROUPS = 8
NEAR = 4
OUTER_FAR = (6, 4, 5, 7)
INNER_FAR = (4, 6, 7, 5)
PARTS = 2
HELD = 0
INNER = 2
ORDER = (0, 4, 5, 1, 6, 2, 3, 7)
HEAD = ("P0", "P1", "Y4", "P2", "P3")
PLAN = (
    ("Y5",),
    ("F4", "Y6"),
    ("F5", "N1", "M4"),
    ("N2", "F6"),
    ("M5", "Y7", "R4"),
    ("N3",),
    ("M6", "R5"),
    ("M1", "F7"),
)
TAIL = ("R6", "M7", "M3", "M2", "M0", "R1", "R7", "R3", "K4")
TAIL += ("R2", "R0", "S0", "K0", "K1", "K5", "K6", "K7", "K3", "K2")
MESH = pl.DeviceIdType.MESH
F32 = jnp.float32
BF16 = jnp.bfloat16


def remote(src, dst, send_sem, recv_sem, device):
    return pltpu.make_async_remote_copy(
        src_ref=src, dst_ref=dst, send_sem=send_sem, recv_sem=recv_sem,
        device_id=device, device_id_type=MESH,
    )


def kernel(
    n, m, cap, slot_rows,
    q_hbm, kv_hbm, sink_hbm, tok_hbm, gain_hbm, routes_hbm, rw_hbm, wg_hbm, wu_hbm, wd_hbm,
    att_hbm, moe_hbm,
    sink_ref, tok_ref, gain_ref, routes_ref, rw_ref, i_sem,
    att_ref, moe_ref, acc, q_ref, wg, wu, wd, kvx, meta, nb, out, piece, xb, hidden, parts, ra, qb, rb, fin, ret,
    comb, pick2,
    o_sem, w_sem, halo_sem, ep_send, ep_recv, y_send, y_recv, c_send, c_recv, d_send, d_recv,
    a_send, a_recv, b_send, b_recv, r_send, r_recv, m_sem, n_send, n_recv,
):
    p = lax.axis_index("ep")
    t = lax.axis_index("tp")
    t1 = t + 1 - 2 * (t % 2)
    t2 = (t + m // 2) % m
    t3 = (t1 + m // 2) % m
    per = n // GROUPS
    near = NEAR * per
    tc = t % 2
    part_width = tok_ref.shape[1] // PARTS
    outer = 1 - (p // (n // 2) + p // (n // 4)) % 2
    width = tok_ref.shape[1]
    hid = wg.shape[1]
    row_count = q_ref.shape[0]
    blocks = row_count // WINDOW

    def xor(a, b):
        total, bit = 0, 1
        while bit < n:
            total = total + ((a // bit + b // bit) % 2) * bit
            bit *= 2
        return total

    loads = [
        pltpu.make_async_copy(wg_hbm, wg, w_sem.at[0]),
        pltpu.make_async_copy(wu_hbm, wu, w_sem.at[1]),
        pltpu.make_async_copy(wd_hbm, wd, w_sem.at[2]),
    ]
    q_load = pltpu.make_async_copy(q_hbm, q_ref, w_sem.at[3])
    kv_load = pltpu.make_async_copy(kv_hbm, kvx.at[pl.ds(WINDOW, row_count)], w_sem.at[4])
    early = [
        pltpu.make_async_copy(source, target, i_sem.at[i])
        for i, (source, target) in enumerate((
            (tok_hbm, tok_ref), (gain_hbm, gain_ref), (routes_hbm, routes_ref), (rw_hbm, rw_ref), (sink_hbm, sink_ref),
        ))
    ]
    for load in early:
        load.start()
    barrier = pltpu.get_barrier_semaphore()
    for s in range(1, n):
        pl.semaphore_signal(barrier, inc=1, device_id=(xor(p, s), t), device_id_type=MESH)
    pl.semaphore_signal(barrier, inc=1, device_id=(p, t1), device_id_type=MESH)
    pl.semaphore_signal(barrier, inc=1, device_id=(p, t2), device_id_type=MESH)

    kv_load.start()
    q_load.start()
    for load in loads:
        load.start()

    for load in early:
        load.wait()
    widened = tok_ref[...].astype(F32)
    scale = lax.rsqrt(jnp.mean(widened * widened, axis=-1, keepdims=True) + EPSILON)
    normed = (widened * scale * gain_ref[...]).astype(BF16)

    own = normed.shape[0]
    nb[0] = normed
    r0 = routes_ref[0:1, :]
    r1 = routes_ref[1:2, :]
    ids = lax.broadcasted_iota(jnp.int32, (max(n, 8), own), 0)
    is0 = ids == r0
    is1 = ids == r1
    member = jnp.where(is0 | is1, 1.0, 0.0).astype(BF16)
    rowi = lax.broadcasted_iota(jnp.int32, (own, own), 0)
    coli = lax.broadcasted_iota(jnp.int32, (own, own), 1)
    before = jnp.where(rowi < coli, 1.0, 0.0).astype(BF16)
    rank = jnp.dot(member, before, preferred_element_type=F32)
    k0 = jnp.sum(jnp.where(is0, rank, 0.0), axis=0, keepdims=True).astype(jnp.int32)
    k1 = jnp.sum(jnp.where(is1, rank, 0.0), axis=0, keepdims=True).astype(jnp.int32)
    e0 = jnp.bitwise_xor(r0, p) * slot_rows + k0
    e1 = jnp.bitwise_xor(r1, p) * slot_rows + k1
    slots = n * slot_rows
    meta[0, 0:1] = e0.astype(F32)
    meta[0, 1:2] = e1.astype(F32)
    meta[0, 2:8] = jnp.zeros((6, own), F32)

    def place(which, count):
        info = meta[which]
        slot_i = lax.broadcasted_iota(jnp.int32, (count * slot_rows, own), 0).astype(F32)
        return slot_i == info[0:1], slot_i == info[1:2]

    in0, in1 = place(0, n)
    pick = jnp.where(in0 | in1, 1.0, 0.0).astype(BF16)
    weight = jnp.where(in0, rw_ref[0:1, :], 0.0) + jnp.where(in1, rw_ref[1:2, :], 0.0)
    for s in range(n):
        comb[s] = weight[s * slot_rows : (s + 1) * slot_rows].astype(BF16)

    def dispatch(s, half=0):
        sem = half * n + s
        return remote(
            out.at[s, half], piece.at[tc, s, half], ep_send.at[sem], ep_recv.at[sem], (xor(p, s), t)
        )

    def halo(to):
        return remote(kvx.at[pl.ds(row_count, WINDOW)], kvx.at[pl.ds(0, WINDOW)], halo_sem.at[0], halo_sem.at[1], (to, t))

    def part(g):
        return pl.ds(g * per, per)

    def y_copy(g):
        return remote(piece.at[tc, part(g), 0], piece.at[tc, part(g), 1], y_send.at[g], y_recv.at[g], (p, t2))

    def c_copy(g, whole):
        here = piece.at[tc, part(g)] if whole else piece.at[tc, part(g), 0]
        return remote(here, here, c_send.at[g], c_recv.at[g], (p, t1))

    tile = min(512, width)
    for c in range(0, width, tile):
        block = jnp.dot(pick, normed[:, c : c + tile], preferred_element_type=F32)
        for s in range(n):
            out[s, 0, :, c : c + tile] = block[s * slot_rows : (s + 1) * slot_rows].astype(BF16)
    piece[tc, 0, 0] = out[0, 0]

    def meta_copy():
        return remote(meta.at[0], meta.at[1], m_sem.at[0], m_sem.at[1], (p, t2))

    def token_copy(i):
        cols = pl.ds(i * tile, tile)
        return remote(nb.at[0, :, cols], nb.at[1, :, cols], n_send.at[i], n_recv.at[i], (p, t2))

    pl.semaphore_wait(barrier, n + 1)

    kv_load.wait()

    @pl.when(p < n - 1)
    def _():
        halo(p + 1).start()

    meta_copy().start()
    for i in range(width // tile - HELD):
        token_copy(i).start()

    def launch(groups, half):
        for g in groups:
            for v in range(max(1, g * per), (g + 1) * per):
                dispatch(v, half).start()

    launch((0, 1), 0)

    @pl.when(outer == 1)
    def _():
        launch(OUTER_FAR, 0)

    launch((2, 3), 0)

    q_load.wait()

    @pl.when(p == 0)
    def _():
        kvx[0:WINDOW, :] = jnp.zeros((WINDOW, kvx.shape[1]), BF16)

    def d_copy(g):
        return remote(piece.at[tc, part(g), 1], piece.at[tc, part(g), 1], d_send.at[g], d_recv.at[g], (p, t1))

    def a_copy(g):
        return remote(parts.at[1 - tc, part(g)], ra.at[part(g)], a_send.at[g], a_recv.at[g], (p, t1))

    def b_copy(g, h):
        cols = pl.ds(h * part_width, part_width)
        return remote(
            qb.at[part(g), :, cols], rb.at[part(g), :, cols], b_send.at[h, g], b_recv.at[h, g], (p, t2)
        )

    def back(s, h):
        cols = pl.ds(h * part_width, part_width)
        return remote(
            fin.at[s, :, cols], ret.at[s, :, cols], r_send.at[h, s], r_recv.at[h, s], (xor(p, s), t)
        )

    def members(g):
        return [g * per + j for j in range(per) if not (isinstance(g, int) and g * per + j == 0)]

    def attention(b):
        head = kvx.shape[1] // 2
        local_heads = q_ref.shape[1] // head
        heads = local_heads * m
        near = kvx[pl.ds(pl.multiple_of(b * WINDOW, WINDOW), 2 * WINDOW), :]
        keys = (near[:, :head].astype(F32) * head ** (-0.5)).astype(BF16)
        ones = jnp.ones((2 * WINDOW, head), BF16)
        values = jnp.concatenate([near[:, head:], ones], axis=1)
        qi = lax.broadcasted_iota(jnp.int32, (WINDOW, 2 * WINDOW), 0)
        kj = lax.broadcasted_iota(jnp.int32, (WINDOW, 2 * WINDOW), 1)
        dist = WINDOW + qi - kj
        first = jnp.where(p + b == 0, WINDOW, 0)
        allowed = (dist >= 0) & (dist < WINDOW) & (kj >= first)
        dist_f = dist.astype(F32)
        at = pl.ds(pl.multiple_of(b * WINDOW, WINDOW), WINDOW)
        for pair in range(0, local_heads, 2):
            both = q_ref[at, pair * head : (pair + 2) * head]
            done = []
            for i in range(2):
                h = pair + i
                scores = lax.dot_general(
                    both[:, i * head : (i + 1) * head], keys, (((1,), (1,)), ((), ())),
                    preferred_element_type=F32,
                )
                ids = jnp.full((1, 2 * WINDOW), t * local_heads + h + 1, jnp.int32).astype(F32)
                slope = jnp.exp2(ids * (-8.0 / heads))
                scores = jnp.where(allowed, scores - slope * dist_f, -1e30)
                sink = sink_ref[h]
                peak = jnp.maximum(jnp.max(scores, axis=-1, keepdims=True), sink)
                weights = jnp.exp(scores - peak).astype(BF16)
                mixed = jnp.dot(weights, values, preferred_element_type=F32)
                total = mixed[:, head : head + 1] + jnp.exp(sink - peak)
                done.append(mixed[:, :head] / total)
            att_ref[at, pair * head : (pair + 2) * head] = jnp.concatenate(done, axis=1).astype(BF16)

    def experts(g):
        for o in range(m):
            for j in range(0, per):
                k = (o * per + j) * slot_rows
                xb[k : k + slot_rows, :] = piece[o // 2, g * per + j, o % 2]
        full = hid // 256 * 256
        x = xb[...]
        for c in range(0, full, 256):
            gate = jnp.dot(x, wg[:, c : c + 256], preferred_element_type=F32)
            up = jnp.dot(x, wu[:, c : c + 256], preferred_element_type=F32)
            hidden[:, c : c + 256] = (gate / (1.0 + jnp.exp(-gate)) * up).astype(BF16)
        if full < hid:
            tail = hid - full
            joint = jnp.concatenate([wg[:, full:], wu[:, full:]], axis=1)
            two = jnp.dot(x, joint, preferred_element_type=F32)
            gate, up = two[:, :tail], two[:, tail:]
            hidden[:, full:] = (gate / (1.0 + jnp.exp(-gate)) * up).astype(BF16)
        h = hidden[...]
        for c in range(0, width, 256):
            product = jnp.dot(h, wd[:, c : c + 256], preferred_element_type=F32)
            for o in range(m):
                for j in range(per):
                    k = (o * per + j) * slot_rows
                    parts[o // 2, g * per + j, o % 2, :, c : c + 256] = product[k : k + slot_rows].astype(BF16)

    across = (((0,), (0,)), ((), ()))
    att_out = pltpu.make_async_copy(att_ref, att_hbm, o_sem.at[0])

    def moe_out(i):
        cols = pl.ds(i * tile, tile)
        return pltpu.make_async_copy(moe_ref.at[:, cols], moe_hbm.at[:, cols], o_sem.at[1 + i])

    def peer(i):
        c = i * tile
        if i == 0:
            meta_copy().wait_recv()
            one0, one1 = place(1, near)
            pick2[0] = jnp.where(one0 | one1, 1.0, 0.0).astype(BF16)
        token_copy(i).wait_recv()
        block = jnp.dot(pick2[0], nb[1, :, c : c + tile], preferred_element_type=F32)
        for v in range(near):
            rows = block[v * slot_rows : (v + 1) * slot_rows].astype(BF16)
            if v > 0:
                out[v, 1, :, c : c + tile] = rows
            else:
                piece[tc, 0, 1, :, c : c + tile] = rows
        if i == INNER:
            @pl.when(outer == 0)
            def _():
                launch(INNER_FAR, 0)

        if i == width // tile - 1:
            launch((0, 1, 2, 3), 1)
            gather(0)

    def queue(i):
        token_copy(i).start()

    def gather(g):
        for v in members(g):
            dispatch(v).wait_recv()
            dispatch(v, 1).wait_recv()
        c_copy(g, True).start()

    def spread(g):
        for v in members(g):
            dispatch(v).wait_recv()
        y_copy(g).start()
        c_copy(g, False).start()

    def forward(g):
        y_copy(g).wait_recv()
        d_copy(g).start()

    def middle(g):
        a_copy(g).wait_recv()
        for h in range(PARTS):
            cols = slice(h * part_width, (h + 1) * part_width)
            for j in range(per):
                v = g * per + j
                mine = parts[tc, v, 1, :, cols].astype(F32)
                qb[v, :, cols] = (mine + ra[v, 1, :, cols].astype(F32)).astype(BF16)
            b_copy(g, h).start()

    def finish(g):
        for h in range(PARTS):
            cols = slice(h * part_width, (h + 1) * part_width)
            b_copy(g, h).wait_recv()
            for j in range(per):
                v = g * per + j
                mine = parts[tc, v, 0, :, cols].astype(F32) + ra[v, 0, :, cols].astype(F32)
                done = (mine + rb[v, :, cols].astype(F32)).astype(BF16)
                if isinstance(v, int) and v == 0:
                    ret[0, :, cols] = done
                else:
                    fin[v, :, cols] = done
                    back(v, h).start()

    def actual(g):
        return g + (g // NEAR) * 2 * outer * (1 - 2 * ((g // 2) % 2))

    begun = [False]

    def combine(g, last):
        for j in range(per):
            v = g * per + j
            for i in range(width // tile):
                if not (isinstance(v, int) and v == 0) and i * tile % part_width == 0:
                    back(v, i * tile // part_width).wait_recv()
                cols = slice(i * tile, (i + 1) * tile)
                term = lax.dot_general(comb[v], ret[v, :, cols], across, preferred_element_type=F32)
                if begun[0]:
                    term = acc[:, cols] + term
                if last and j == per - 1:
                    moe_ref[:, cols] = term.astype(BF16)
                    moe_out(i).start()
                else:
                    acc[:, cols] = term
            begun[0] = True

    def arrive(g, close):
        c_copy(g, close).wait_recv()
        if not close:
            d_copy(g).wait_recv()

    def drain(_):
        @pl.when(p < n - 1)
        def _():
            halo(p + 1).wait_send()

        meta_copy().wait_send()
        for i in range(width // tile):
            token_copy(i).wait_send()
        for s in range(1, n):
            dispatch(s).wait_send()
            if s < near:
                dispatch(s, 1).wait_send()
        for g in range(GROUPS):
            c_copy(g, g < NEAR).wait_send()
            a_copy(g).wait_send()
            for h in range(PARTS):
                b_copy(g, h).wait_send()
            if g >= NEAR:
                y_copy(g).wait_send()
                d_copy(g).wait_send()

    acts = dict(S=drain, P=peer, Q=queue, N=gather, Y=spread, F=forward, M=middle, R=finish)

    def run(ops, last=False):
        for op in ops:
            g = int(op[1:])
            close = g < NEAR
            final = last and op == ops[-1]
            where = g if close else actual(g)
            if op[0] == "K":
                combine(where, final)
            elif op[0] == "E":
                arrive(where, close)
            else:
                acts[op[0]](where)

    @pl.loop(0, blocks)
    def _(b):
        @pl.when((b == blocks - 1) & (p > 0))
        def _():
            halo((p + 1) % n).wait_recv()

        attention(blocks - 1 - b)

    att_out.start()
    for load in loads:
        load.wait()

    run(HEAD)

    def step(it, code):
        for k, ops in enumerate(PLAN):
            @pl.when(it == k)
            def _(ops=ops + ("E%d" % ORDER[k],)):
                run(ops)

        g = actual(code % GROUPS)
        experts(g)
        a_copy(g).start()
        return code // GROUPS

    lax.fori_loop(0, GROUPS, step, jnp.int32(sum(g * GROUPS**k for k, g in enumerate(ORDER))))
    run(TAIL, True)
    att_out.wait()
    for i in range(width // tile):
        moe_out(i).wait()

    for s in range(1, n):
        for h in range(PARTS):
            back(s, h).wait_send()


def settle(attended_hbm, moe_hbm, attended_out, moe_out, attended_ref, moe_ref, sem):
    loads, stores = [], []
    for source, held, target in ((attended_hbm, attended_ref, attended_out), (moe_hbm, moe_ref, moe_out)):
        step = source.shape[0] // 2
        for i in range(2):
            at = pl.ds(i * step, step)
            loads.append(pltpu.make_async_copy(source.at[at], held.at[at], sem.at[0, len(loads)]))
            stores.append(pltpu.make_async_copy(held.at[at], target.at[at], sem.at[1, len(stores)]))
    for load in loads:
        load.start()
    for load, store in zip(loads, stores):
        load.wait()
        store.start()
    for store in stores:
        store.wait()


def local(n, m, queries, keys_values, sinks, tokens_b, norm_gain, routes, route_weights, gate_weight, up_weight, down_weight):
    own_rows, top_count = routes.shape
    width = tokens_b.shape[1]
    cap = max(2, 5 * own_rows * top_count // (4 * n))
    slot_rows = (cap + 7) // 8 * 8
    hid = gate_weight.shape[2]
    per = n // GROUPS
    rows = m * per * slot_rows
    tiles = width // min(512, width)
    hbm = pl.BlockSpec(memory_space=pltpu.HBM)
    dma = pltpu.SemaphoreType.DMA
    attended, moe = pl.pallas_call(
        functools.partial(kernel, n, m, cap, slot_rows),
        out_shape=(
            jax.ShapeDtypeStruct(queries.shape, BF16),
            jax.ShapeDtypeStruct(tokens_b.shape, BF16),
        ),
        in_specs=[hbm] * 10,
        out_specs=(hbm, hbm),
        scratch_shapes=[
            pltpu.SMEM(sinks.shape, F32),
            pltpu.VMEM(tokens_b.shape, BF16),
            pltpu.VMEM((1, width), F32),
            pltpu.VMEM((top_count, own_rows), jnp.int32),
            pltpu.VMEM((top_count, own_rows), F32),
            dma((5,)),
            pltpu.VMEM(queries.shape, BF16),
            pltpu.VMEM(tokens_b.shape, BF16),
            pltpu.VMEM(tokens_b.shape, F32),
            pltpu.VMEM(queries.shape, BF16),
            pltpu.VMEM((width, hid), BF16),
            pltpu.VMEM((width, hid), BF16),
            pltpu.VMEM((hid, width), BF16),
            pltpu.VMEM((keys_values.shape[0] + WINDOW, keys_values.shape[2]), BF16),
            pltpu.VMEM((2, 8, own_rows), F32),
            pltpu.VMEM((2, own_rows, width), BF16),
            pltpu.VMEM((n, 2, slot_rows, width), BF16),
            pltpu.VMEM((2, n, 2, slot_rows, width), BF16),
            pltpu.VMEM((rows, width), BF16),
            pltpu.VMEM((rows, hid), BF16),
            pltpu.VMEM((2, n, 2, slot_rows, width), BF16),
            pltpu.VMEM((n, 2, slot_rows, width), BF16),
            pltpu.VMEM((n, slot_rows, width), BF16),
            pltpu.VMEM((n, slot_rows, width), BF16),
            pltpu.VMEM((n, slot_rows, width), BF16),
            pltpu.VMEM((n, slot_rows, width), BF16),
            pltpu.VMEM((n, slot_rows, own_rows), BF16),
            pltpu.VMEM((1, NEAR * per * slot_rows, own_rows), BF16),
            dma((1 + tiles,)), dma((5,)), dma((2,)), dma((2 * n,)), dma((2 * n,)),
            dma((GROUPS,)), dma((GROUPS,)), dma((GROUPS,)), dma((GROUPS,)), dma((GROUPS,)), dma((GROUPS,)),
            dma((GROUPS,)), dma((GROUPS,)), dma((PARTS, GROUPS)), dma((PARTS, GROUPS)),
            dma((PARTS, n)), dma((PARTS, n)),
            dma((2,)), dma((tiles,)), dma((tiles,)),
        ],
        compiler_params=pltpu.CompilerParams(
            collective_id=0, has_side_effects=True, vmem_limit_bytes=62 * 1024 * 1024
        ),
    )(
        queries,
        keys_values.reshape(keys_values.shape[0], keys_values.shape[2]),
        sinks,
        tokens_b,
        norm_gain.reshape(1, width),
        routes.T,
        route_weights.T,
        gate_weight.reshape(width, hid),
        up_weight.reshape(width, hid),
        down_weight.reshape(hid, width),
    )
    return pl.pallas_call(
        settle,
        out_shape=(
            jax.ShapeDtypeStruct(queries.shape, BF16),
            jax.ShapeDtypeStruct(tokens_b.shape, BF16),
        ),
        in_specs=[hbm, hbm],
        out_specs=(hbm, hbm),
        scratch_shapes=[
            pltpu.VMEM(queries.shape, BF16),
            pltpu.VMEM(tokens_b.shape, BF16),
            dma((2, 4)),
        ],
    )(attended, moe)


def solution(mesh):
    in_specs = (
        P("ep", "tp"),
        P("ep", "tp", None),
        P("tp"),
        P(("ep", "tp"), None),
        P(),
        P(("ep", "tp"), None),
        P(("ep", "tp"), None),
        P("ep", None, "tp"),
        P("ep", None, "tp"),
        P("ep", "tp", None),
    )
    out_specs = (P("ep", "tp"), P(("ep", "tp"), None))
    body = functools.partial(local, mesh.shape["ep"], mesh.shape["tp"])
    return jax.shard_map(body, mesh=mesh, in_specs=in_specs, out_specs=out_specs, check_vma=False)
```
